128 devices in a mesh: ep: 64 (over z, y, x), tp: 2 (over core).
Axes of the slice: x: 4, y: 4, z: 4, core: 2. Of those that a mesh axis runs over, the one named last changes fastest.
Arguments:
- tokens: bfloat16 [1024, 2048], P('ep'), may hold values from -6 to 6
- mix_gain: float32 [2048], replicated, may hold values from 0.1 to 1.9
- w_query: bfloat16 [2048, 1024], P(None, 'tp'), may hold values from -0.125 to 0.125
- w_forget: bfloat16 [2048, 1024], P(None, 'tp'), may hold values from -0.125 to 0.125
- w_input: bfloat16 [2048, 1024], P(None, 'tp'), may hold values from -0.125 to 0.125
- w_outgate: bfloat16 [2048, 1024], P(None, 'tp'), may hold values from -0.125 to 0.125
- decay_floor: float32 [1024], P('tp'), may hold values from 0 to 0.9
- head_gain: float32 [128], replicated, may hold values from 0.1 to 1.9
- prev_state: float32 [1024, 8, 128, 128], P('ep', 'tp'), may hold values from -4 to 4
- w_output: bfloat16 [1024, 2048], P('tp'), may hold values from -0.1875 to 0.1875
- moe_gain: float32 [2048], replicated, may hold values from 0.1 to 1.9
- route_ids: int32 [1024, 2], P('ep'), may hold values from 0 to 31, all different within a row; in each aligned block of 16 rows (0 to 15, 16 to 31, ...) at most 8 rows name the same one
- route_logits: float32 [1024, 2], P('ep'), may hold values from -6 to 6
- w_exp_gate: bfloat16 [64, 2048, 1536], P('ep', None, 'tp'), may hold values from -0.125 to 0.125
- w_exp_up: bfloat16 [64, 2048, 1536], P('ep', None, 'tp'), may hold values from -0.125 to 0.125
- w_exp_down: bfloat16 [64, 1536, 2048], P('ep', 'tp'), may hold values from -0.109375 to 0.109375
Outputs:
- layer_out: bfloat16 [1024, 2048], P('ep')
- new_state: float32 [1024, 8, 128, 128], P('ep', 'tp')
The draws below stay inside these ranges and needn't reach their ends.
Inputs may be any that keep to these rules, and one draw needn't show every extreme that they name: `route_ids`: each row names 2 different experts; within the rows of one device no expert is named more than 8 times, and in every draw some expert is named exactly 8 times in some device's rows.
All inputs are finite; a program needn't handle non-finite values.
Results may differ from the reference program's by a relative error of at most 0.014.
Values may be sent and summed in bfloat16 or wider, within the bound.
A program may use at most 128 MiB of HBM per device.

```python
import math
import jax
import jax.numpy as jnp
import numpy as np
from jax import lax

WIDTH = 2048
HEADS = 8
HEAD_DIM = 128
MIX_WIDTH = 1024
HIDDEN_SIZE = 3072
TOP_K = 2
SEQ_DEV = 16
SEQS = 1024
EXPERTS = 32
CAPACITY = 8
N_EP = 64
N_TP = 2


def level_of(stream_key, extent, cuts, least, largest):
    level = 1.0
    for dim, blocks in cuts:
        heights = jax.random.uniform(jax.random.fold_in(jax.random.fold_in(stream_key, 6), dim), (blocks,), jnp.float32, least / len(cuts), largest / len(cuts))
        level = level * jnp.repeat(jnp.exp(heights), extent[dim] // blocks).reshape((-1,) + (1,) * (len(extent) - 1 - dim))
    return level


def deal_out(stream_key, own, number, rows, count, top, limit, slope):
    ranking = jax.random.permutation(stream_key, count)
    packed, usual = load_shares(count, rows * top, limit, slope, True), load_shares(count, rows * top, limit, slope, False)
    places = jnp.arange(count)

    def named(lengths, rotation):
        used = int((lengths > 0).sum())
        fixed = max(1, used // 4)
        moved = fixed + (places - fixed + rotation * (used - fixed)) % max(1, count - fixed)
        return jnp.zeros((count,), jnp.int32).at[ranking[jnp.where(places < fixed, places, moved)]].set(jnp.asarray(lengths, jnp.int32))

    lengths = jnp.where(number % 4 == 0, named(packed, number // 4), named(usual, number - number // 4 - 1))
    mixed = jax.random.permutation(jax.random.fold_in(own, 3), count)
    source_of, taker = mixed[0:count // 2 * 2:2], mixed[1:count // 2 * 2:2]
    room = jnp.minimum(lengths[source_of] - 1, limit - lengths[taker]) // 2
    room = jnp.where((source_of == ranking[0]) | (taker == ranking[0]) | (lengths[taker] == 0), 0, jnp.maximum(room, 0))
    moved = jax.random.randint(jax.random.fold_in(own, 4), (count // 2,), 0, 1 << 20) % (room + 1)
    lengths = lengths.at[source_of].add(-moved).at[taker].add(moved)
    members = jnp.searchsorted(jnp.cumsum(lengths), jnp.arange(rows * top), side="right").astype(jnp.int32)
    listing = members.reshape(top, rows).T
    listing = listing[jax.random.permutation(jax.random.fold_in(own, 1), rows)]
    rotation = jax.random.randint(jax.random.fold_in(own, 2), (rows, 1), 0, top)
    return jnp.take_along_axis(listing, (jnp.arange(top)[None, :] + rotation) % top, axis=1)


def load_shares(amount, total, limit, lean, full):
    weights = [(1 << 20) // math.isqrt(grade ** lean) + 1 for grade in range(1, amount + 1)]
    largest = limit if full else min(limit, max(-(-total // amount), total * weights[0] // sum(weights)))
    least = 1 if total - largest >= amount - 1 else 0
    given, surplus = [largest] + [least] * (amount - 1), total - largest - least * (amount - 1)
    while surplus > 0:
        movable = [i for i in range(1, amount) if given[i] < largest] or [i for i in range(1, amount) if given[i] < limit]
        whole, remaining = sum([weights[i] for i in movable]), surplus
        for i in movable:
            addition = min(limit - given[i], max(1, remaining * weights[i] // whole), surplus)
            given[i] = given[i] + addition
            surplus = surplus - addition
    return np.array(given)


def normal_values(key, dims, spread, reach, pieces=(), held_as=jnp.bfloat16):
    array = jax.random.normal(key, dims, jnp.float32) * spread
    if len(pieces) > 0:
        array = level_of(key, dims, pieces, -0.22, 0.18) * array
    return jnp.clip(array, min=-reach, max=reach).astype(held_as)


def setup_inputs(seed: int = 0) -> dict:
    key_of = jax.random.split(jax.random.key(seed), 17)
    tokens = normal_values(key_of[0], (SEQS, WIDTH), 1.0, 6.0, ((0, 64),))
    mix_gain = jnp.clip(1.0 + 0.18 * jax.random.normal(key_of[1], (WIDTH,), jnp.float32), 0.1, 1.9)
    w_query = normal_values(key_of[2], (WIDTH, MIX_WIDTH), WIDTH ** -0.5, 0.125, ((1, 2),))
    w_forget = normal_values(key_of[3], (WIDTH, MIX_WIDTH), WIDTH ** -0.5, 0.125, ((1, 2),))
    w_input = normal_values(key_of[4], (WIDTH, MIX_WIDTH), WIDTH ** -0.5, 0.125, ((1, 2),))
    w_outgate = normal_values(key_of[5], (WIDTH, MIX_WIDTH), WIDTH ** -0.5, 0.125, ((1, 2),))
    decay_floor = jnp.clip(0.9 * jax.random.uniform(key_of[6], (MIX_WIDTH,), jnp.float32) ** level_of(key_of[6], (MIX_WIDTH,), ((0, 2),), -0.2, 0.2), 0.0, 0.9)
    head_gain = jnp.clip(1.0 + 0.18 * jax.random.normal(key_of[7], (HEAD_DIM,), jnp.float32), 0.1, 1.9)
    prev_state = normal_values(key_of[8], (SEQS, HEADS, HEAD_DIM, HEAD_DIM), 0.3, 4.0, ((0, 64), (1, 2)), jnp.float32)
    w_output = normal_values(key_of[9], (MIX_WIDTH, WIDTH), MIX_WIDTH ** -0.5, 0.1875, ((0, 2),))
    moe_gain = jnp.clip(1.0 + 0.18 * jax.random.normal(key_of[10], (WIDTH,), jnp.float32), 0.1, 1.9)
    route_ids_keys = jax.random.split(jax.random.fold_in(key_of[11], 1), SEQS // SEQ_DEV)
    route_ids_turns = jax.random.permutation(jax.random.fold_in(key_of[11], 3), SEQS // SEQ_DEV)
    route_ids = jax.vmap(lambda own, number: deal_out(jax.random.fold_in(key_of[11], 2), own, number, SEQ_DEV, EXPERTS, TOP_K, CAPACITY, 2))(route_ids_keys, route_ids_turns).reshape((SEQS, TOP_K))
    route_logits = normal_values(key_of[12], (SEQS, TOP_K), 1.5, 6.0, ((0, 64),), jnp.float32)
    w_exp_gate = normal_values(key_of[13], (2 * EXPERTS, WIDTH, HIDDEN_SIZE // 2), WIDTH ** -0.5, 0.125, ((0, 64), (2, 2)))
    w_exp_up = normal_values(key_of[14], (2 * EXPERTS, WIDTH, HIDDEN_SIZE // 2), WIDTH ** -0.5, 0.125, ((0, 64), (2, 2)))
    w_exp_down = normal_values(key_of[15], (2 * EXPERTS, HIDDEN_SIZE // 2, WIDTH), HIDDEN_SIZE ** -0.5, 0.109375, ((0, 64), (1, 2)))
    return {"tokens": tokens, "mix_gain": mix_gain, "w_query": w_query, "w_forget": w_forget, "w_input": w_input, "w_outgate": w_outgate, "decay_floor": decay_floor, "head_gain": head_gain, "prev_state": prev_state, "w_output": w_output, "moe_gain": moe_gain, "route_ids": route_ids, "route_logits": route_logits, "w_exp_gate": w_exp_gate, "w_exp_up": w_exp_up, "w_exp_down": w_exp_down}


epsilon = 1e-06

def rms_scale(values, gains):
    return values * lax.rsqrt(lax.optimization_barrier(jnp.mean(values * values, axis=-1, keepdims=True)) + epsilon) * gains

def reference(tokens, mix_gain, w_query, w_forget, w_input, w_outgate, decay_floor, head_gain, prev_state, w_output, moe_gain, route_ids, route_logits, w_exp_gate, w_exp_up, w_exp_down):
    seq_count = tokens.shape[0]
    residual = tokens.astype(jnp.float32)
    normed = rms_scale(residual, mix_gain).astype(jnp.bfloat16)
    query_part = jnp.dot(normed, w_query, preferred_element_type=jnp.float32).reshape(seq_count, HEADS, HEAD_DIM)
    forget_pre = jnp.dot(normed, w_forget, preferred_element_type=jnp.float32).reshape(seq_count, HEADS, HEAD_DIM)
    value_part = jnp.dot(normed, w_input, preferred_element_type=jnp.float32).reshape(seq_count, HEADS, HEAD_DIM)
    outgate_pre = jnp.dot(normed, w_outgate, preferred_element_type=jnp.float32).reshape(seq_count, HEADS, HEAD_DIM)
    floor_rate = decay_floor.reshape(HEADS, HEAD_DIM)
    forget = floor_rate + (1.0 - floor_rate) * jax.nn.sigmoid(forget_pre)
    key_part = (1.0 - floor_rate) * jax.nn.sigmoid(-forget_pre)
    new_state = forget[..., None] * prev_state + key_part[..., None] * value_part[:, :, None, :]
    readout = lax.optimization_barrier(jnp.sum(query_part[..., None] * new_state, axis=2))
    gated = (rms_scale(readout, head_gain) * jax.nn.silu(outgate_pre)).reshape(seq_count, MIX_WIDTH).astype(jnp.bfloat16)
    head_width = MIX_WIDTH // N_TP
    mixed_out = jnp.zeros((seq_count, WIDTH), jnp.float32)
    for part_index in range(N_TP):
        lower = part_index * head_width
        partial_out = jnp.dot(gated[:, lower:lower + head_width], w_output[lower:lower + head_width], preferred_element_type=jnp.float32).astype(jnp.bfloat16)
        mixed_out = mixed_out + lax.optimization_barrier(partial_out).astype(jnp.float32)
    middle = (residual + mixed_out).astype(jnp.bfloat16)
    normed_two = rms_scale(middle.astype(jnp.float32), moe_gain).astype(jnp.bfloat16)
    pair_expert = route_ids.reshape(-1).astype(jnp.int32)
    pair_count = pair_expert.shape[0]
    onehot = (pair_expert[:, None] == jnp.arange(EXPERTS, dtype=jnp.int32)[None, :]).astype(jnp.int32)
    slot_rank = lax.optimization_barrier(jnp.sum((jnp.cumsum(onehot, axis=0) - onehot) * onehot, axis=1)).astype(jnp.int32)
    slot_limit = N_EP * CAPACITY
    slot_table = jnp.zeros((EXPERTS, slot_limit), jnp.int32).at[pair_expert, slot_rank].set(jnp.arange(pair_count, dtype=jnp.int32) // TOP_K)
    half_hidden = w_exp_gate.shape[2]
    piece_hidden = half_hidden // N_TP

    def half_expert(half_index):
        slot_rows = normed_two[slot_table[half_index // 2]]
        gate_pre = jnp.dot(slot_rows, w_exp_gate[half_index], preferred_element_type=jnp.float32)
        up_pre = jnp.dot(slot_rows, w_exp_up[half_index], preferred_element_type=jnp.float32)
        activated = (jax.nn.silu(gate_pre) * up_pre).astype(jnp.bfloat16)
        down_all = w_exp_down[half_index]
        running = jnp.zeros((slot_limit, WIDTH), jnp.float32)
        for part_index in range(N_TP):
            lower = part_index * piece_hidden
            partial_down = jnp.dot(activated[:, lower:lower + piece_hidden], down_all[lower:lower + piece_hidden], preferred_element_type=jnp.float32).astype(jnp.bfloat16)
            running = running + lax.optimization_barrier(partial_down).astype(jnp.float32)
        return running.astype(jnp.bfloat16)
    halves = lax.map(half_expert, jnp.arange(2 * EXPERTS, dtype=jnp.int32))
    first_half = halves[2 * pair_expert, slot_rank].astype(jnp.float32)
    second = halves[2 * pair_expert + 1, slot_rank].astype(jnp.float32)
    both_halves = (first_half + second).reshape(seq_count, TOP_K, WIDTH)
    weights = jax.nn.sigmoid(route_logits - jnp.flip(route_logits, axis=1))
    expert_sum = lax.optimization_barrier(jnp.sum(weights[..., None] * both_halves, axis=1))
    layer_out = (middle.astype(jnp.float32) + expert_sum).astype(jnp.bfloat16)
    return (layer_out, new_state)
```

```python
import functools

import jax
import jax.numpy as jnp
import numpy as np
from jax import lax
from jax.experimental import pallas as pl
from jax.experimental.pallas import tpu as pltpu
from jax.sharding import PartitionSpec as P

MESH = pl.DeviceIdType.MESH
SIDE = 4
CHIPS = SIDE**3
EXPERTS = CHIPS // 2
CAP = 8
CHUNKS = 4
PER = CHIPS // CHUNKS
ROWS = PER * CAP
SEQ = 16
WIDTH = 2048
HALF = WIDTH // 2
HEADS = 4
HEAD = 128
MIX = HEADS * HEAD
HID = 768
EPS = 1e-6
BF = jnp.bfloat16
F32 = jnp.float32


def hops(offset):
    return sum(min(v, SIDE - v) for v in offset)


def offset_order():
    every = [(z, y, x) for z in range(SIDE) for y in range(SIDE) for x in range(SIDE)]
    order = []
    for k in range(CHUNKS):
        mine = [o for o in every if sum(o) % SIDE == k]
        order += sorted(mine, key=lambda o: (o != (0, 0, 0), -hops(o), o))
    return order


OFFSETS = offset_order()


def slot_table():
    packed = [z * 16 + y * 4 + x for z, y, x in OFFSETS]
    return np.repeat(np.array(packed, np.int32), CAP)[None, :]


def rms(values, gains):
    return values * lax.rsqrt(jnp.mean(values * values, axis=-1, keepdims=True) + EPS) * gains


def layer_kernel(
    tokens,
    mix_gain,
    floor,
    head_gain,
    moe_gain,
    ids,
    ids_t,
    logits,
    table,
    w_query,
    w_forget,
    w_input,
    w_outgate,
    prev,
    w_output,
    w_gate,
    w_up,
    w_down,
    out,
    forget_t,
    value_out,
    wq_v,
    wf_v,
    wi_v,
    wg_v,
    prev_v,
    wo_v,
    eg_v,
    eu_v,
    ed_v,
    readout_v,
    part_own,
    part_sib,
    n2_v,
    middle_v,
    outgoing,
    inbox,
    down_send,
    down_recv,
    ret_out,
    ret_in,
    final,
    load_sem,
    prev_sem,
    expert_sem,
    pair_sem,
    disp_send,
    disp_recv,
    fwd_send,
    fwd_recv,
    down_sems,
    down_recv_sems,
    ret_send,
    ret_recv,
):
    me = lax.axis_index("ep")
    c = lax.axis_index("tp")
    other = 1 - c
    z, y, x = lax.div(me, 16), lax.rem(lax.div(me, 4), 4), lax.rem(me, 4)
    z_to = [lax.rem(z + d, 4) * 16 for d in range(4)]
    y_to = [lax.rem(y + d, 4) * 4 for d in range(4)]
    x_to = [lax.rem(x + d, 4) for d in range(4)]

    def ahead(o):
        return z_to[o[0]] + y_to[o[1]] + x_to[o[2]]

    def behind(o):
        return z_to[-o[0] % 4] + y_to[-o[1] % 4] + x_to[-o[2] % 4]

    def to_sibling(src, dst, send, recv):
        return pltpu.make_async_remote_copy(
            src_ref=src, dst_ref=dst, send_sem=send, recv_sem=recv, device_id={"tp": other}, device_id_type=MESH
        )

    barrier = pltpu.get_barrier_semaphore()
    pl.semaphore_signal(barrier, inc=1, device_id={"tp": other}, device_id_type=MESH)
    for o in OFFSETS[1:]:
        pl.semaphore_signal(barrier, inc=1, device_id={"ep": ahead(o)}, device_id_type=MESH)

    loads = [
        pltpu.make_async_copy(src, dst, load_sem.at[i])
        for i, (src, dst) in enumerate(
            ((w_forget, wf_v), (w_query, wq_v), (w_input, wi_v), (w_outgate, wg_v), (w_output, wo_v))
        )
    ]
    prev_loads = [
        pltpu.make_async_copy(prev.at[pl.ds(4 * i, 4)], prev_v.at[pl.ds(4 * i, 4)], prev_sem.at[i]) for i in range(4)
    ]
    loads[0].start()
    loads[1].start()
    loads[2].start()
    for copy in prev_loads:
        copy.start()
    loads[3].start()
    loads[4].start()

    ids_col = [ids[:, k : k + 1] for k in range(2)]
    ids_row = [ids_t[k : k + 1, :] for k in range(2)]
    rows16 = lax.broadcasted_iota(jnp.int32, (SEQ, SEQ), 0)
    cols16 = lax.broadcasted_iota(jnp.int32, (SEQ, SEQ), 1)

    def rank_col(k):
        same = (ids_col[k] == ids_row[0]).astype(jnp.int32) + (ids_col[k] == ids_row[1]).astype(jnp.int32)
        return jnp.sum(jnp.where(cols16 < rows16, same, 0), axis=1, keepdims=True)

    def rank_row(k):
        same = (ids_row[k] == ids_col[0]).astype(jnp.int32) + (ids_row[k] == ids_col[1]).astype(jnp.int32)
        return jnp.sum(jnp.where(rows16 < cols16, same, 0), axis=0, keepdims=True)

    slot_row = lax.broadcasted_iota(jnp.int32, (EXPERTS * CAP, SEQ), 0)
    disp = jnp.zeros((EXPERTS * CAP, SEQ), F32)
    for k in range(2):
        disp = jnp.where(slot_row == ids_row[k] * CAP + rank_row(k), 1.0, disp)
    disp = disp.astype(BF)

    tab = table[...]
    chip = (((tab >> 4) + z) & 3) * 16 + ((((tab >> 2) & 3) + y) & 3) * 4 + (((tab & 3) + x) & 3)
    slot_lane = lax.broadcasted_iota(jnp.int32, (1, CHIPS * CAP), 1)
    slot_key = (chip >> 1) * CAP + (slot_lane & (CAP - 1))
    comb = jnp.zeros((SEQ, CHIPS * CAP), F32)
    for k in range(2):
        weight = jax.nn.sigmoid(logits[:, k : k + 1] - logits[:, 1 - k : 2 - k])
        comb = jnp.where(slot_key == ids_col[k] * CAP + rank_col(k), weight, comb)
    comb_hi = comb.astype(BF)
    comb_lo = (comb - comb_hi.astype(F32)).astype(BF)
    comb = jnp.concatenate([comb_hi, comb_lo], axis=0)

    residual = tokens[...].astype(F32)
    normed = rms(residual, mix_gain[...]).astype(BF)
    loads[0].wait()
    forget_pre = jnp.dot(normed, wf_v[...], preferred_element_type=F32)
    low = floor[...]
    forget = low + (1.0 - low) * jax.nn.sigmoid(forget_pre)
    key = (1.0 - low) * jax.nn.sigmoid(-forget_pre)
    loads[1].wait()
    query = jnp.dot(normed, wq_v[...], preferred_element_type=F32)
    query_forget = query * forget
    query_key = query * key
    loads[2].wait()
    value = jnp.dot(normed, wi_v[...], preferred_element_type=F32)
    value_out[...] = value
    for h in range(HEADS):
        lanes = slice(h * HEAD, (h + 1) * HEAD)
        forget_t[h] = forget[:, lanes].T
    for copy in prev_loads:
        copy.wait()
    expert_loads = [
        pltpu.make_async_copy(src.at[0], dst, expert_sem.at[i])
        for i, (src, dst) in enumerate(((w_gate, eg_v), (w_up, eu_v), (w_down, ed_v)))
    ]
    for copy in expert_loads:
        copy.start()
    for h in range(HEADS):
        lanes = slice(h * HEAD, (h + 1) * HEAD)
        columns = query_forget[:, lanes].T
        for s in range(SEQ):
            readout_v[s : s + 1, lanes] = jnp.sum(columns[:, s : s + 1] * prev_v[s, h], axis=0, keepdims=True)
    loads[3].wait()
    outgate_pre = jnp.dot(normed, wg_v[...], preferred_element_type=F32)
    gate = outgate_pre * jax.nn.sigmoid(outgate_pre)
    gated = []
    for h in range(HEADS):
        lanes = slice(h * HEAD, (h + 1) * HEAD)
        dotted = jnp.sum(query_key[:, lanes], axis=1, keepdims=True)
        readout = readout_v[:, lanes] + dotted * value[:, lanes]
        gated.append((rms(readout, head_gain[...]) * gate[:, lanes]).astype(BF))
    gated = jnp.concatenate(gated, axis=1)
    loads[4].wait()
    part_own[...] = jnp.dot(gated, wo_v[...], preferred_element_type=F32).astype(BF)

    pl.semaphore_wait(barrier, CHIPS)
    swap = to_sibling(part_own, part_sib, pair_sem.at[0], pair_sem.at[1])
    swap.start()
    swap.wait()
    middle = (residual + (part_own[...].astype(F32) + part_sib[...].astype(F32))).astype(BF)
    middle_v[...] = middle
    n2_v[...] = rms(middle.astype(F32), moe_gain[...]).astype(BF)
    mine = pl.ds(pl.multiple_of(c * HALF, HALF), HALF)
    theirs = pl.ds(pl.multiple_of(other * HALF, HALF), HALF)
    rows = jnp.dot(disp, n2_v[:, mine], preferred_element_type=F32)
    outgoing[...] = rows.reshape(EXPERTS, CAP, HALF).astype(BF)

    def slots(ref, k, first=0):
        return ref.at[pl.ds(k * PER + first, PER - first)]

    def wait_for(ref, k, sem):
        first = 1 if k == 0 else 0
        pltpu.make_async_copy(slots(ref, k, first), slots(ref, k, first), sem).wait()

    for i, o in enumerate(OFFSETS):
        if i == 0:
            continue
        to = ahead(o)
        pltpu.make_async_remote_copy(
            src_ref=outgoing.at[lax.div(to, 2)],
            dst_ref=inbox.at[c, i],
            send_sem=disp_send.at[i // PER],
            recv_sem=disp_recv.at[i // PER],
            device_id={"ep": to},
            device_id_type=MESH,
        ).start()
    inbox[c, 0] = outgoing[lax.div(me, 2)]

    def flat(values):
        return values.astype(F32).reshape(ROWS, HALF).astype(BF)

    def finish(k):
        down_swaps[k].wait()
        total = own_down[k] + down_recv[k].astype(F32)
        ret_out[pl.ds(k * PER, PER)] = total.reshape(PER, CAP, HALF).astype(BF)
        for j in range(PER):
            i = k * PER + j
            if i == 0:
                ret_in[0] = ret_out[0]
                continue
            pltpu.make_async_remote_copy(
                src_ref=ret_out.at[i],
                dst_ref=ret_in.at[i],
                send_sem=ret_send.at[k],
                recv_sem=ret_recv.at[k],
                device_id={"ep": behind(OFFSETS[i])},
                device_id_type=MESH,
            ).start()

    down_swaps, own_down = [], []
    for k in range(CHUNKS):
        wait_for(inbox.at[c], k, disp_recv.at[k])
        forward = to_sibling(slots(inbox.at[c], k), slots(inbox.at[c], k), fwd_send.at[k], fwd_recv.at[k])
        forward.start()
        if k == 0:
            for copy in expert_loads:
                copy.wait()
        rows = flat(inbox[c, pl.ds(k * PER, PER)])
        gate_pre = jnp.dot(rows, eg_v[mine, :], preferred_element_type=F32)
        up_pre = jnp.dot(rows, eu_v[mine, :], preferred_element_type=F32)
        if k > 0:
            finish(k - 1)
        forward.wait()
        rows = flat(inbox[other, pl.ds(k * PER, PER)])
        gate_pre = gate_pre + jnp.dot(rows, eg_v[theirs, :], preferred_element_type=F32)
        up_pre = up_pre + jnp.dot(rows, eu_v[theirs, :], preferred_element_type=F32)
        activated = (gate_pre * jax.nn.sigmoid(gate_pre) * up_pre).astype(BF)
        down_send[k] = jnp.dot(activated, ed_v[:, theirs], preferred_element_type=F32).astype(BF)
        swap = to_sibling(down_send.at[k], down_recv.at[k], down_sems.at[k], down_recv_sems.at[k])
        swap.start()
        down_swaps.append(swap)
        own_down.append(jnp.dot(activated, ed_v[:, mine], preferred_element_type=F32))
    finish(CHUNKS - 1)

    total = jnp.zeros((2 * SEQ, HALF), F32)
    for k in range(CHUNKS):
        wait_for(ret_in, k, ret_recv.at[k])
        total += jnp.dot(
            comb[:, k * ROWS : (k + 1) * ROWS], flat(ret_in[pl.ds(k * PER, PER)]), preferred_element_type=F32
        )
    expert_sum = total[:SEQ] + total[SEQ:]
    final[c] = (middle_v[:, mine].astype(F32) + expert_sum).astype(BF)
    swap = to_sibling(final.at[c], final.at[c], pair_sem.at[2], pair_sem.at[3])
    swap.start()
    swap.wait()
    out[:, :HALF] = final[0]
    out[:, HALF:] = final[1]
    for k in range(CHUNKS):
        wait_for(inbox.at[c], k, disp_send.at[k])
        wait_for(ret_in, k, ret_send.at[k])


def state_kernel(forget_t, value, prev, new):
    for s in range(SEQ):
        vector = value[s : s + 1, :]
        new[s, 0] = vector + forget_t[0, :, s : s + 1] * (prev[s, 0] - vector)


def on_device(
    tokens,
    mix_gain,
    w_query,
    w_forget,
    w_input,
    w_outgate,
    decay_floor,
    head_gain,
    prev_state,
    w_output,
    moe_gain,
    route_ids,
    route_logits,
    w_exp_gate,
    w_exp_up,
    w_exp_down,
):
    vmem = pl.BlockSpec(memory_space=pltpu.VMEM)
    hbm = pl.BlockSpec(memory_space=pl.ANY)
    dma = pltpu.SemaphoreType.DMA
    layer_out, forget_t, value = pl.pallas_call(
        layer_kernel,
        name="layer",
        out_shape=(
            jax.ShapeDtypeStruct((SEQ, WIDTH), BF),
            jax.ShapeDtypeStruct((HEADS, HEAD, SEQ), F32),
            jax.ShapeDtypeStruct((SEQ, MIX), F32),
        ),
        in_specs=[vmem] * 9 + [hbm] * 9,
        out_specs=(vmem,) * 3,
        scratch_shapes=[
            pltpu.VMEM((WIDTH, MIX), BF),
            pltpu.VMEM((WIDTH, MIX), BF),
            pltpu.VMEM((WIDTH, MIX), BF),
            pltpu.VMEM((WIDTH, MIX), BF),
            pltpu.VMEM((SEQ, HEADS, HEAD, HEAD), F32),
            pltpu.VMEM((MIX, WIDTH), BF),
            pltpu.VMEM((WIDTH, HID), BF),
            pltpu.VMEM((WIDTH, HID), BF),
            pltpu.VMEM((HID, WIDTH), BF),
            pltpu.VMEM((SEQ, MIX), F32),
            pltpu.VMEM((SEQ, WIDTH), BF),
            pltpu.VMEM((SEQ, WIDTH), BF),
            pltpu.VMEM((SEQ, WIDTH), BF),
            pltpu.VMEM((SEQ, WIDTH), BF),
            pltpu.VMEM((EXPERTS, CAP, HALF), BF),
            pltpu.VMEM((2, CHIPS, CAP, HALF), BF),
            pltpu.VMEM((CHUNKS, ROWS, HALF), BF),
            pltpu.VMEM((CHUNKS, ROWS, HALF), BF),
            pltpu.VMEM((CHIPS, CAP, HALF), BF),
            pltpu.VMEM((CHIPS, CAP, HALF), BF),
            pltpu.VMEM((2, SEQ, HALF), BF),
            dma((5,)),
            dma((4,)),
            dma((3,)),
            dma((4,)),
            dma((CHUNKS,)),
            dma((CHUNKS,)),
            dma((CHUNKS,)),
            dma((CHUNKS,)),
            dma((CHUNKS,)),
            dma((CHUNKS,)),
            dma((CHUNKS,)),
            dma((CHUNKS,)),
        ],
        compiler_params=pltpu.CompilerParams(
            collective_id=0, has_side_effects=True, vmem_limit_bytes=60 * 1024 * 1024
        ),
    )(
        tokens,
        mix_gain[None, :],
        decay_floor[None, :],
        head_gain[None, :],
        moe_gain[None, :],
        route_ids,
        route_ids.T,
        route_logits,
        jnp.asarray(slot_table()),
        w_query,
        w_forget,
        w_input,
        w_outgate,
        prev_state,
        w_output,
        w_exp_gate,
        w_exp_up,
        w_exp_down,
    )
    by_head = pl.BlockSpec((SEQ, 1, HEAD, HEAD), lambda h: (0, h, 0, 0))
    new_state = pl.pallas_call(
        state_kernel,
        name="state",
        grid=(HEADS,),
        out_shape=jax.ShapeDtypeStruct((SEQ, HEADS, HEAD, HEAD), F32),
        in_specs=[
            pl.BlockSpec((1, HEAD, SEQ), lambda h: (h, 0, 0)),
            pl.BlockSpec((SEQ, HEAD), lambda h: (0, h)),
            by_head,
        ],
        out_specs=by_head,
        cost_estimate=pl.CostEstimate(flops=3 * SEQ * MIX * HEAD, bytes_accessed=8 * SEQ * MIX * HEAD, transcendentals=0),
    )(forget_t, value, prev_state)
    return (layer_out, new_state)


def solution(mesh):
    placed = (
        P("ep", None),
        P(),
        P(None, "tp"),
        P(None, "tp"),
        P(None, "tp"),
        P(None, "tp"),
        P("tp"),
        P(),
        P("ep", "tp", None, None),
        P("tp", None),
        P(),
        P("ep", None),
        P("ep", None),
        P("ep", None, "tp"),
        P("ep", None, "tp"),
        P("ep", "tp", None),
    )
    return jax.shard_map(
        on_device,
        mesh=mesh,
        in_specs=placed,
        out_specs=(P("ep", None), P("ep", "tp", None, None)),
        check_vma=False,
    )
```

```python
import functools

import jax
import jax.numpy as jnp
import numpy as np
from jax import lax
from jax.experimental import pallas as pl
from jax.experimental.pallas import tpu as pltpu
from jax.sharding import PartitionSpec as P

MESH = pl.DeviceIdType.MESH
SIDE = 4
CHIPS = SIDE**3
EXPERTS = CHIPS // 2
CAP = 8
CHUNKS = 4
PER = CHIPS // CHUNKS
ROWS = PER * CAP
OWN = CHIPS - PER
SEQ = 16
WIDTH = 2048
HALF = WIDTH // 2
HEADS = 4
HEAD = 128
MIX = HEADS * HEAD
HID = 768
EPS = 1e-6
BF = jnp.bfloat16
F32 = jnp.float32


def hops(offset):
    return sum(min(v, SIDE - v) for v in offset)


def offset_order():
    every = [(z, y, x) for z in range(SIDE) for y in range(SIDE) for x in range(SIDE)]
    order = sorted(every[1:], key=lambda o: (-hops(o), sum(o) % SIDE, o))
    order.insert(OWN, (0, 0, 0))
    return order


OFFSETS = offset_order()


def slot_table():
    packed = [z * 16 + y * 4 + x for z, y, x in OFFSETS]
    return np.repeat(np.array(packed, np.int32), CAP)[None, :]


def rms(values, gains):
    return values * lax.rsqrt(jnp.mean(values * values, axis=-1, keepdims=True) + EPS) * gains


def layer_kernel(
    tokens_h,
    mix_gain_h,
    floor_h,
    head_gain_h,
    moe_gain_h,
    ids_h,
    logits_h,
    table_h,
    w_query,
    w_forget,
    w_input,
    w_outgate,
    prev,
    w_output,
    w_gate,
    w_up,
    w_down,
    out,
    new_state,
    tokens,
    mix_gain,
    floor,
    head_gain,
    moe_gain,
    ids_t,
    logits_t,
    table,
    wq_v,
    wf_v,
    wi_v,
    wg_v,
    prev_v,
    wo_v,
    eg_v,
    eu_v,
    ed_v,
    readout_v,
    part_own,
    part_sib,
    n2_v,
    middle_v,
    outgoing,
    inbox,
    down_send,
    down_recv,
    ret_out,
    ret_in,
    final,
    small_sem,
    load_sem,
    prev_sem,
    expert_sem,
    pair_sem,
    disp_send,
    disp_recv,
    fwd_send,
    fwd_recv,
    down_sems,
    down_recv_sems,
    ret_send,
    ret_recv,
):
    me = lax.axis_index("ep")
    c = lax.axis_index("tp")
    other = 1 - c
    z, y, x = lax.div(me, 16), lax.rem(lax.div(me, 4), 4), lax.rem(me, 4)
    z_to = [lax.rem(z + d, 4) * 16 for d in range(4)]
    y_to = [lax.rem(y + d, 4) * 4 for d in range(4)]
    x_to = [lax.rem(x + d, 4) for d in range(4)]

    def ahead(o):
        return z_to[o[0]] + y_to[o[1]] + x_to[o[2]]

    def behind(o):
        return z_to[-o[0] % 4] + y_to[-o[1] % 4] + x_to[-o[2] % 4]

    def to_sibling(src, dst, send, recv):
        return pltpu.make_async_remote_copy(
            src_ref=src, dst_ref=dst, send_sem=send, recv_sem=recv, device_id={"tp": other}, device_id_type=MESH
        )

    barrier = pltpu.get_barrier_semaphore()
    pl.semaphore_signal(barrier, inc=1, device_id={"tp": other}, device_id_type=MESH)
    for o in OFFSETS[:OWN] + OFFSETS[OWN + 1 :]:
        pl.semaphore_signal(barrier, inc=1, device_id={"ep": ahead(o)}, device_id_type=MESH)

    small = [
        pltpu.make_async_copy(src, dst, small_sem.at[i])
        for i, (src, dst) in enumerate(
            (
                (tokens_h, tokens),
                (mix_gain_h, mix_gain),
                (floor_h, floor),
                (head_gain_h, head_gain),
                (moe_gain_h, moe_gain),
                (ids_h, ids_t),
                (logits_h, logits_t),
                (table_h, table),
            )
        )
    ]
    loads = [
        pltpu.make_async_copy(src, dst, load_sem.at[i])
        for i, (src, dst) in enumerate(
            ((w_forget, wf_v), (w_query, wq_v), (w_input, wi_v), (w_outgate, wg_v), (w_output, wo_v))
        )
    ]
    prev_loads = [
        pltpu.make_async_copy(prev.at[pl.ds(4 * i, 4)], prev_v.at[pl.ds(4 * i, 4)], prev_sem.at[i]) for i in range(4)
    ]
    for copy in small:
        copy.start()
    loads[0].start()
    loads[1].start()
    loads[2].start()
    for copy in prev_loads:
        copy.start()
    loads[3].start()
    loads[4].start()
    for copy in small:
        copy.wait()

    rows16 = lax.broadcasted_iota(jnp.int32, (SEQ, SEQ), 0)
    cols16 = lax.broadcasted_iota(jnp.int32, (SEQ, SEQ), 1)

    def column(row):
        return jnp.sum(jnp.where(rows16 == cols16, row, jnp.zeros_like(row)), axis=1, keepdims=True)

    ids_row = [ids_t[k : k + 1, :] for k in range(2)]
    ids_col = [column(row) for row in ids_row]

    def rank_col(k):
        same = (ids_col[k] == ids_row[0]).astype(jnp.int32) + (ids_col[k] == ids_row[1]).astype(jnp.int32)
        return jnp.sum(jnp.where(cols16 < rows16, same, 0), axis=1, keepdims=True)

    def rank_row(k):
        same = (ids_row[k] == ids_col[0]).astype(jnp.int32) + (ids_row[k] == ids_col[1]).astype(jnp.int32)
        return jnp.sum(jnp.where(rows16 < cols16, same, 0), axis=0, keepdims=True)

    slot_row = lax.broadcasted_iota(jnp.int32, (EXPERTS * CAP, SEQ), 0)
    disp = jnp.zeros((EXPERTS * CAP, SEQ), F32)
    for k in range(2):
        disp = jnp.where(slot_row == ids_row[k] * CAP + rank_row(k), 1.0, disp)
    disp = disp.astype(BF)

    tab = table[...]
    chip = (((tab >> 4) + z) & 3) * 16 + ((((tab >> 2) & 3) + y) & 3) * 4 + (((tab & 3) + x) & 3)
    slot_lane = lax.broadcasted_iota(jnp.int32, (1, CHIPS * CAP), 1)
    slot_key = (chip >> 1) * CAP + (slot_lane & (CAP - 1))
    comb = jnp.zeros((SEQ, CHIPS * CAP), F32)
    for k in range(2):
        weight = column(jax.nn.sigmoid(logits_t[k : k + 1, :] - logits_t[1 - k : 2 - k, :]))
        comb = jnp.where(slot_key == ids_col[k] * CAP + rank_col(k), weight, comb)
    comb_hi = comb.astype(BF)
    comb_lo = (comb - comb_hi.astype(F32)).astype(BF)
    comb = jnp.concatenate([comb_hi, comb_lo], axis=0)

    residual = tokens[...].astype(F32)
    normed = rms(residual, mix_gain[...]).astype(BF)
    loads[0].wait()
    forget_pre = jnp.dot(normed, wf_v[...], preferred_element_type=F32)
    low = floor[...]
    forget = low + (1.0 - low) * jax.nn.sigmoid(forget_pre)
    key = (1.0 - low) * jax.nn.sigmoid(-forget_pre)
    loads[1].wait()
    query = jnp.dot(normed, wq_v[...], preferred_element_type=F32)
    query_forget = query * forget
    query_key = query * key
    loads[2].wait()
    value = jnp.dot(normed, wi_v[...], preferred_element_type=F32)
    for copy in prev_loads:
        copy.wait()
    expert_loads = [
        pltpu.make_async_copy(src.at[0], dst, expert_sem.at[i])
        for i, (src, dst) in enumerate(((w_gate, eg_v), (w_up, eu_v), (w_down, ed_v)))
    ]
    for copy in expert_loads:
        copy.start()
    for h in range(HEADS):
        lanes = slice(h * HEAD, (h + 1) * HEAD)
        columns = query_forget[:, lanes].T
        for s in range(SEQ):
            readout_v[s : s + 1, lanes] = jnp.sum(columns[:, s : s + 1] * prev_v[s, h], axis=0, keepdims=True)
    loads[3].wait()
    outgate_pre = jnp.dot(normed, wg_v[...], preferred_element_type=F32)
    gate = outgate_pre * jax.nn.sigmoid(outgate_pre)
    gated = []
    for h in range(HEADS):
        lanes = slice(h * HEAD, (h + 1) * HEAD)
        dotted = jnp.sum(query_key[:, lanes], axis=1, keepdims=True)
        readout = readout_v[:, lanes] + dotted * value[:, lanes]
        gated.append((rms(readout, head_gain[...]) * gate[:, lanes]).astype(BF))
    gated = jnp.concatenate(gated, axis=1)
    loads[4].wait()
    part_own[...] = jnp.dot(gated, wo_v[...], preferred_element_type=F32).astype(BF)

    pl.semaphore_wait(barrier, CHIPS)
    swap = to_sibling(part_own, part_sib, pair_sem.at[0], pair_sem.at[1])
    swap.start()
    swap.wait()
    middle = (residual + (part_own[...].astype(F32) + part_sib[...].astype(F32))).astype(BF)
    middle_v[...] = middle
    n2_v[...] = rms(middle.astype(F32), moe_gain[...]).astype(BF)
    mine = pl.ds(pl.multiple_of(c * HALF, HALF), HALF)
    theirs = pl.ds(pl.multiple_of(other * HALF, HALF), HALF)
    rows = jnp.dot(disp, n2_v[:, mine], preferred_element_type=F32)
    outgoing[...] = rows.reshape(EXPERTS, CAP, HALF).astype(BF)

    def slots(ref, k, first=0):
        return ref.at[pl.ds(k * PER + first, PER - first)]

    def wait_for(ref, k, sem):
        first = 1 if k == OWN // PER else 0
        pltpu.make_async_copy(slots(ref, k, first), slots(ref, k, first), sem).wait()

    for i, o in enumerate(OFFSETS):
        if i == OWN:
            continue
        to = ahead(o)
        pltpu.make_async_remote_copy(
            src_ref=outgoing.at[lax.div(to, 2)],
            dst_ref=inbox.at[c, i],
            send_sem=disp_send.at[i // PER],
            recv_sem=disp_recv.at[i // PER],
            device_id={"ep": to},
            device_id_type=MESH,
        ).start()
    inbox[c, OWN] = outgoing[lax.div(me, 2)]

    for h in range(HEADS):
        lanes = slice(h * HEAD, (h + 1) * HEAD)
        columns = forget[:, lanes].T
        for s in range(SEQ):
            vector = value[s : s + 1, lanes]
            new_state[s, h] = vector + columns[:, s : s + 1] * (prev_v[s, h] - vector)

    def flat(values):
        return values.astype(F32).reshape(ROWS, HALF).astype(BF)

    def finish(k):
        down_swaps[k].wait()
        total = own_down[k] + down_recv[k].astype(F32)
        ret_out[pl.ds(k * PER, PER)] = total.reshape(PER, CAP, HALF).astype(BF)
        for j in range(PER):
            i = k * PER + j
            if i == OWN:
                ret_in[OWN] = ret_out[OWN]
                continue
            pltpu.make_async_remote_copy(
                src_ref=ret_out.at[i],
                dst_ref=ret_in.at[i],
                send_sem=ret_send.at[k],
                recv_sem=ret_recv.at[k],
                device_id={"ep": behind(OFFSETS[i])},
                device_id_type=MESH,
            ).start()

    down_swaps, own_down = [], []
    for k in range(CHUNKS):
        wait_for(inbox.at[c], k, disp_recv.at[k])
        forward = to_sibling(slots(inbox.at[c], k), slots(inbox.at[c], k), fwd_send.at[k], fwd_recv.at[k])
        forward.start()
        if k == 0:
            for copy in expert_loads:
                copy.wait()
        rows = flat(inbox[c, pl.ds(k * PER, PER)])
        gate_pre = jnp.dot(rows, eg_v[mine, :], preferred_element_type=F32)
        up_pre = jnp.dot(rows, eu_v[mine, :], preferred_element_type=F32)
        if k > 0:
            finish(k - 1)
        forward.wait()
        rows = flat(inbox[other, pl.ds(k * PER, PER)])
        gate_pre = gate_pre + jnp.dot(rows, eg_v[theirs, :], preferred_element_type=F32)
        up_pre = up_pre + jnp.dot(rows, eu_v[theirs, :], preferred_element_type=F32)
        activated = (gate_pre * jax.nn.sigmoid(gate_pre) * up_pre).astype(BF)
        down_send[k] = jnp.dot(activated, ed_v[:, theirs], preferred_element_type=F32).astype(BF)
        swap = to_sibling(down_send.at[k], down_recv.at[k], down_sems.at[k], down_recv_sems.at[k])
        swap.start()
        down_swaps.append(swap)
        own_down.append(jnp.dot(activated, ed_v[:, mine], preferred_element_type=F32))
    finish(CHUNKS - 1)

    total = jnp.zeros((2 * SEQ, HALF), F32)
    for k in range(CHUNKS):
        wait_for(ret_in, k, ret_recv.at[k])
        total += jnp.dot(
            comb[:, k * ROWS : (k + 1) * ROWS], flat(ret_in[pl.ds(k * PER, PER)]), preferred_element_type=F32
        )
    expert_sum = total[:SEQ] + total[SEQ:]
    final[c] = (middle_v[:, mine].astype(F32) + expert_sum).astype(BF)
    swap = to_sibling(final.at[c], final.at[c], pair_sem.at[2], pair_sem.at[3])
    swap.start()
    swap.wait()
    out[:, :HALF] = final[0]
    out[:, HALF:] = final[1]
    for k in range(CHUNKS):
        wait_for(inbox.at[c], k, disp_send.at[k])
        wait_for(ret_in, k, ret_send.at[k])


def on_device(
    tokens,
    mix_gain,
    w_query,
    w_forget,
    w_input,
    w_outgate,
    decay_floor,
    head_gain,
    prev_state,
    w_output,
    moe_gain,
    route_ids,
    route_logits,
    w_exp_gate,
    w_exp_up,
    w_exp_down,
):
    vmem = pl.BlockSpec(memory_space=pltpu.VMEM)
    hbm = pl.BlockSpec(memory_space=pltpu.HBM)
    dma = pltpu.SemaphoreType.DMA
    layer_out, new_state = pl.pallas_call(
        layer_kernel,
        name="layer",
        out_shape=(
            pltpu.VMEM((SEQ, WIDTH), BF),
            pltpu.VMEM((SEQ, HEADS, HEAD, HEAD), F32),
        ),
        in_specs=[hbm] * 17,
        out_specs=(vmem,) * 2,
        scratch_shapes=[
            pltpu.VMEM((SEQ, WIDTH), BF),
            pltpu.VMEM((1, WIDTH), F32),
            pltpu.VMEM((1, MIX), F32),
            pltpu.VMEM((1, HEAD), F32),
            pltpu.VMEM((1, WIDTH), F32),
            pltpu.VMEM((2, SEQ), jnp.int32),
            pltpu.VMEM((2, SEQ), F32),
            pltpu.VMEM((1, CHIPS * CAP), jnp.int32),
            pltpu.VMEM((WIDTH, MIX), BF),
            pltpu.VMEM((WIDTH, MIX), BF),
            pltpu.VMEM((WIDTH, MIX), BF),
            pltpu.VMEM((WIDTH, MIX), BF),
            pltpu.VMEM((SEQ, HEADS, HEAD, HEAD), F32),
            pltpu.VMEM((MIX, WIDTH), BF),
            pltpu.VMEM((WIDTH, HID), BF),
            pltpu.VMEM((WIDTH, HID), BF),
            pltpu.VMEM((HID, WIDTH), BF),
            pltpu.VMEM((SEQ, MIX), F32),
            pltpu.VMEM((SEQ, WIDTH), BF),
            pltpu.VMEM((SEQ, WIDTH), BF),
            pltpu.VMEM((SEQ, WIDTH), BF),
            pltpu.VMEM((SEQ, WIDTH), BF),
            pltpu.VMEM((EXPERTS, CAP, HALF), BF),
            pltpu.VMEM((2, CHIPS, CAP, HALF), BF),
            pltpu.VMEM((CHUNKS, ROWS, HALF), BF),
            pltpu.VMEM((CHUNKS, ROWS, HALF), BF),
            pltpu.VMEM((CHIPS, CAP, HALF), BF),
            pltpu.VMEM((CHIPS, CAP, HALF), BF),
            pltpu.VMEM((2, SEQ, HALF), BF),
            dma((8,)),
            dma((5,)),
            dma((4,)),
            dma((3,)),
            dma((4,)),
            dma((CHUNKS,)),
            dma((CHUNKS,)),
            dma((CHUNKS,)),
            dma((CHUNKS,)),
            dma((CHUNKS,)),
            dma((CHUNKS,)),
            dma((CHUNKS,)),
            dma((CHUNKS,)),
        ],
        compiler_params=pltpu.CompilerParams(
            collective_id=0, has_side_effects=True, vmem_limit_bytes=62750720
        ),
    )(
        tokens,
        mix_gain[None, :],
        decay_floor[None, :],
        head_gain[None, :],
        moe_gain[None, :],
        route_ids.T,
        route_logits.T,
        jnp.asarray(slot_table()),
        w_query,
        w_forget,
        w_input,
        w_outgate,
        prev_state,
        w_output,
        w_exp_gate,
        w_exp_up,
        w_exp_down,
    )
    return (layer_out, new_state)


def solution(mesh):
    placed = (
        P("ep", None),
        P(),
        P(None, "tp"),
        P(None, "tp"),
        P(None, "tp"),
        P(None, "tp"),
        P("tp"),
        P(),
        P("ep", "tp", None, None),
        P("tp", None),
        P(),
        P("ep", None),
        P("ep", None),
        P("ep", None, "tp"),
        P("ep", None, "tp"),
        P("ep", "tp", None),
    )
    return jax.shard_map(
        on_device,
        mesh=mesh,
        in_specs=placed,
        out_specs=(P("ep", None), P("ep", "tp", None, None)),
        check_vma=False,
    )
```

```python
import functools

import jax
import jax.numpy as jnp
import numpy as np
from jax import lax
from jax.experimental import pallas as pl
from jax.experimental.pallas import tpu as pltpu
from jax.sharding import PartitionSpec as P

MESH = pl.DeviceIdType.MESH
SIDE = 4
CHIPS = SIDE**3
EXPERTS = CHIPS // 2
CAP = 8
SIZES = (16, 16, 16, 16)
STARTS = tuple(sum(SIZES[:k]) for k in range(len(SIZES)))
CHUNKS = len(SIZES)
OWN = STARTS[-1]
SEQ = 16
WIDTH = 2048
HALF = WIDTH // 2
HEADS = 4
HEAD = 128
MIX = HEADS * HEAD
HID = 768
EPS = 1e-6
AHEAD = 6
BF = jnp.bfloat16
F32 = jnp.float32


def hops(offset):
    return sum(min(v, SIDE - v) for v in offset)


def offset_order():
    every = [(z, y, x) for z in range(SIDE) for y in range(SIDE) for x in range(SIDE)]
    order = sorted(every[1:], key=lambda o: ((sum(o) - 1) % SIDE, -hops(o), o))
    order.insert(OWN, (0, 0, 0))
    return order


OFFSETS = offset_order()


def slot_table():
    packed = [z * 16 + y * 4 + x for z, y, x in OFFSETS]
    return np.repeat(np.array(packed, np.int32), CAP)[None, :]


def rms(values, gains):
    return values * lax.rsqrt(jnp.mean(values * values, axis=-1, keepdims=True) + EPS) * gains


def halves(src, dst):
    size = src.shape[0] // 2
    return [(src.at[pl.ds(i * size, size)], dst.at[pl.ds(i * size, size)]) for i in range(2)]


def layer_kernel(
    tokens_h,
    mix_gain_h,
    floor_h,
    head_gain_h,
    moe_gain_h,
    ids_h,
    logits_h,
    table_h,
    w_query,
    w_forget,
    w_input,
    w_outgate,
    prev,
    w_output,
    w_gate,
    w_up,
    w_down,
    out,
    new_state,
    tokens,
    mix_gain,
    floor,
    head_gain,
    moe_gain,
    ids_t,
    logits_t,
    table,
    wq_v,
    wf_v,
    wi_v,
    wg_v,
    prev_v,
    wo_v,
    eg_v,
    eu_v,
    ed_v,
    readout_v,
    part_own,
    part_sib,
    n2_v,
    middle_v,
    outgoing,
    inbox,
    down_send,
    down_recv,
    ret_out,
    ret_in,
    final,
    small_sem,
    load_sem,
    pair_sem,
    disp_send,
    disp_recv,
    fwd_send,
    fwd_recv,
    down_sems,
    down_recv_sems,
    ret_send,
    ret_recv,
):
    me = lax.axis_index("ep")
    c = lax.axis_index("tp")
    other = 1 - c
    z, y, x = lax.div(me, 16), lax.rem(lax.div(me, 4), 4), lax.rem(me, 4)
    z_to = [lax.rem(z + d, 4) * 16 for d in range(4)]
    y_to = [lax.rem(y + d, 4) * 4 for d in range(4)]
    x_to = [lax.rem(x + d, 4) for d in range(4)]

    def ahead(o):
        return z_to[o[0]] + y_to[o[1]] + x_to[o[2]]

    def behind(o):
        return z_to[-o[0] % 4] + y_to[-o[1] % 4] + x_to[-o[2] % 4]

    def to_sibling(src, dst, send, recv):
        return pltpu.make_async_remote_copy(
            src_ref=src, dst_ref=dst, send_sem=send, recv_sem=recv, device_id={"tp": other}, device_id_type=MESH
        )

    barrier = pltpu.get_barrier_semaphore()
    pl.semaphore_signal(barrier, inc=1, device_id={"tp": other}, device_id_type=MESH)
    for o in OFFSETS[:OWN] + OFFSETS[OWN + 1 :]:
        pl.semaphore_signal(barrier, inc=1, device_id={"ep": ahead(o)}, device_id_type=MESH)

    small = [
        pltpu.make_async_copy(src, dst, small_sem.at[i])
        for i, (src, dst) in enumerate(
            (
                (tokens_h, tokens),
                (mix_gain_h, mix_gain),
                (floor_h, floor),
                (head_gain_h, head_gain),
                (moe_gain_h, moe_gain),
                (ids_h, ids_t),
                (logits_h, logits_t),
                (table_h, table),
            )
        )
    ]
    parts = []
    for src, dst in ((w_forget, wf_v), (w_query, wq_v)):
        parts += halves(src, dst)
    parts += [(prev.at[pl.ds(4 * i, 4)], prev_v.at[pl.ds(4 * i, 4)]) for i in range(4)]
    for src, dst in ((w_input, wi_v), (w_outgate, wg_v), (w_output, wo_v)):
        parts += halves(src, dst)
    parts += [(w_gate.at[0], eg_v), (w_up.at[0], eu_v), (w_down.at[0], ed_v)]
    loads = [pltpu.make_async_copy(src, dst, load_sem.at[i]) for i, (src, dst) in enumerate(parts)]
    expert_loads = loads[14:]

    def arrive(first, count):
        for i in range(first, first + count):
            loads[i].wait()
            if i + AHEAD < len(loads):
                loads[i + AHEAD].start()

    for copy in small:
        copy.start()
    for copy in loads[:AHEAD]:
        copy.start()
    for copy in small:
        copy.wait()

    rows16 = lax.broadcasted_iota(jnp.int32, (SEQ, SEQ), 0)
    cols16 = lax.broadcasted_iota(jnp.int32, (SEQ, SEQ), 1)

    def column(row):
        return jnp.sum(jnp.where(rows16 == cols16, row, jnp.zeros_like(row)), axis=1, keepdims=True)

    ids_row = [ids_t[k : k + 1, :] for k in range(2)]
    ids_col = [column(row) for row in ids_row]

    def rank_col(k):
        same = (ids_col[k] == ids_row[0]).astype(jnp.int32) + (ids_col[k] == ids_row[1]).astype(jnp.int32)
        return jnp.sum(jnp.where(cols16 < rows16, same, 0), axis=1, keepdims=True)

    def rank_row(k):
        same = (ids_row[k] == ids_col[0]).astype(jnp.int32) + (ids_row[k] == ids_col[1]).astype(jnp.int32)
        return jnp.sum(jnp.where(rows16 < cols16, same, 0), axis=0, keepdims=True)

    slot_row = lax.broadcasted_iota(jnp.int32, (EXPERTS * CAP, SEQ), 0)
    disp = jnp.zeros((EXPERTS * CAP, SEQ), F32)
    for k in range(2):
        disp = jnp.where(slot_row == ids_row[k] * CAP + rank_row(k), 1.0, disp)
    disp = disp.astype(BF)

    tab = table[...]
    chip = (((tab >> 4) + z) & 3) * 16 + ((((tab >> 2) & 3) + y) & 3) * 4 + (((tab & 3) + x) & 3)
    slot_lane = lax.broadcasted_iota(jnp.int32, (1, CHIPS * CAP), 1)
    slot_key = (chip >> 1) * CAP + (slot_lane & (CAP - 1))
    comb = jnp.zeros((SEQ, CHIPS * CAP), F32)
    for k in range(2):
        weight = column(jax.nn.sigmoid(logits_t[k : k + 1, :] - logits_t[1 - k : 2 - k, :]))
        comb = jnp.where(slot_key == ids_col[k] * CAP + rank_col(k), weight, comb)
    comb_hi = comb.astype(BF)
    comb_lo = (comb - comb_hi.astype(F32)).astype(BF)
    comb = jnp.concatenate([comb_hi, comb_lo], axis=0)

    residual = tokens[...].astype(F32)
    normed = rms(residual, mix_gain[...]).astype(BF)
    arrive(0, 2)
    forget_pre = jnp.dot(normed, wf_v[...], preferred_element_type=F32)
    low = floor[...]
    forget = low + (1.0 - low) * jax.nn.sigmoid(forget_pre)
    key = (1.0 - low) * jax.nn.sigmoid(-forget_pre)
    arrive(2, 2)
    query = jnp.dot(normed, wq_v[...], preferred_element_type=F32)
    query_forget = query * forget
    query_key = query * key
    columns = [query_forget[:, h * HEAD : (h + 1) * HEAD].T for h in range(HEADS)]
    for part in range(4):
        arrive(4 + part, 1)
        for s in range(4 * part, 4 * part + 4):
            for h in range(HEADS):
                lanes = slice(h * HEAD, (h + 1) * HEAD)
                readout_v[s : s + 1, lanes] = jnp.sum(columns[h][:, s : s + 1] * prev_v[s, h], axis=0, keepdims=True)
    arrive(8, 2)
    value = jnp.dot(normed, wi_v[...], preferred_element_type=F32)
    arrive(10, 2)
    outgate_pre = jnp.dot(normed, wg_v[...], preferred_element_type=F32)
    gate = outgate_pre * jax.nn.sigmoid(outgate_pre)
    gated = []
    for h in range(HEADS):
        lanes = slice(h * HEAD, (h + 1) * HEAD)
        dotted = jnp.sum(query_key[:, lanes], axis=1, keepdims=True)
        readout = readout_v[:, lanes] + dotted * value[:, lanes]
        gated.append((rms(readout, head_gain[...]) * gate[:, lanes]).astype(BF))
    gated = jnp.concatenate(gated, axis=1)
    arrive(12, 2)
    part_own[...] = jnp.dot(gated, wo_v[...], preferred_element_type=F32).astype(BF)

    pl.semaphore_wait(barrier, CHIPS)
    swap = to_sibling(part_own, part_sib, pair_sem.at[0], pair_sem.at[1])
    swap.start()
    swap.wait()
    middle = (residual + (part_own[...].astype(F32) + part_sib[...].astype(F32))).astype(BF)
    middle_v[...] = middle
    n2_v[...] = rms(middle.astype(F32), moe_gain[...]).astype(BF)
    mine = pl.ds(pl.multiple_of(c * HALF, HALF), HALF)
    theirs = pl.ds(pl.multiple_of(other * HALF, HALF), HALF)
    rows = jnp.dot(disp, n2_v[:, mine], preferred_element_type=F32)
    outgoing[...] = rows.reshape(EXPERTS, CAP, HALF).astype(BF)

    def slots(ref, k, first=0):
        return ref.at[pl.ds(STARTS[k] + first, SIZES[k] - first)]

    def chunk_of(i):
        return max(k for k in range(CHUNKS) if STARTS[k] <= i)

    def wait_for(ref, k, sem):
        first = 1 if k == chunk_of(OWN) else 0
        pltpu.make_async_copy(slots(ref, k, first), slots(ref, k, first), sem).wait()

    for i, o in enumerate(OFFSETS):
        if i == OWN:
            continue
        to = ahead(o)
        pltpu.make_async_remote_copy(
            src_ref=outgoing.at[lax.div(to, 2)],
            dst_ref=inbox.at[c, i],
            send_sem=disp_send.at[chunk_of(i)],
            recv_sem=disp_recv.at[chunk_of(i)],
            device_id={"ep": to},
            device_id_type=MESH,
        ).start()
    inbox[c, OWN] = outgoing[lax.div(me, 2)]

    for h in range(HEADS):
        lanes = slice(h * HEAD, (h + 1) * HEAD)
        columns = forget[:, lanes].T
        for s in range(SEQ):
            vector = value[s : s + 1, lanes]
            new_state[s, h] = vector + columns[:, s : s + 1] * (prev_v[s, h] - vector)

    def rows_of(k):
        return pl.ds(STARTS[k] * CAP, SIZES[k] * CAP)

    def flat(values):
        return values.astype(F32).reshape(values.shape[0] * CAP, HALF).astype(BF)

    def finish(k):
        down_swaps[k].wait()
        total = own_down[k] + down_recv[rows_of(k)].astype(F32)
        ret_out[pl.ds(STARTS[k], SIZES[k])] = total.reshape(SIZES[k], CAP, HALF).astype(BF)
        for i in range(STARTS[k], STARTS[k] + SIZES[k]):
            if i == OWN:
                ret_in[OWN] = ret_out[OWN]
                continue
            pltpu.make_async_remote_copy(
                src_ref=ret_out.at[i],
                dst_ref=ret_in.at[i],
                send_sem=ret_send.at[k],
                recv_sem=ret_recv.at[k],
                device_id={"ep": behind(OFFSETS[i])},
                device_id_type=MESH,
            ).start()

    down_swaps, own_down = [], []
    for k in range(CHUNKS):
        wait_for(inbox.at[c], k, disp_recv.at[k])
        forward = to_sibling(slots(inbox.at[c], k), slots(inbox.at[c], k), fwd_send.at[k], fwd_recv.at[k])
        forward.start()
        if k == 0:
            for copy in expert_loads:
                copy.wait()
        rows = flat(inbox[c, pl.ds(STARTS[k], SIZES[k])])
        gate_pre = jnp.dot(rows, eg_v[mine, :], preferred_element_type=F32)
        up_pre = jnp.dot(rows, eu_v[mine, :], preferred_element_type=F32)
        if k > 0:
            finish(k - 1)
        forward.wait()
        rows = flat(inbox[other, pl.ds(STARTS[k], SIZES[k])])
        gate_pre = gate_pre + jnp.dot(rows, eg_v[theirs, :], preferred_element_type=F32)
        up_pre = up_pre + jnp.dot(rows, eu_v[theirs, :], preferred_element_type=F32)
        activated = (gate_pre * jax.nn.sigmoid(gate_pre) * up_pre).astype(BF)
        down_send[rows_of(k)] = jnp.dot(activated, ed_v[:, theirs], preferred_element_type=F32).astype(BF)
        swap = to_sibling(down_send.at[rows_of(k)], down_recv.at[rows_of(k)], down_sems.at[k], down_recv_sems.at[k])
        swap.start()
        down_swaps.append(swap)
        own_down.append(jnp.dot(activated, ed_v[:, mine], preferred_element_type=F32))
    finish(CHUNKS - 1)

    total = jnp.zeros((2 * SEQ, HALF), F32)
    for k in range(CHUNKS):
        wait_for(ret_in, k, ret_recv.at[k])
        total += jnp.dot(
            comb[:, STARTS[k] * CAP : (STARTS[k] + SIZES[k]) * CAP],
            flat(ret_in[pl.ds(STARTS[k], SIZES[k])]),
            preferred_element_type=F32,
        )
    expert_sum = total[:SEQ] + total[SEQ:]
    final[c] = (middle_v[:, mine].astype(F32) + expert_sum).astype(BF)
    swap = to_sibling(final.at[c], final.at[c], pair_sem.at[2], pair_sem.at[3])
    swap.start()
    swap.wait()
    out[:, :HALF] = final[0]
    out[:, HALF:] = final[1]
    for k in range(CHUNKS):
        wait_for(inbox.at[c], k, disp_send.at[k])
        wait_for(ret_in, k, ret_send.at[k])


def deliver_kernel(made, state, out, new_state, sem):
    copies = [pltpu.make_async_copy(made, out, sem.at[4])]
    for i in range(4):
        part = pl.ds(4 * i, 4)
        copies.append(pltpu.make_async_copy(state.at[part], new_state.at[part], sem.at[i]))
    for copy in copies:
        copy.start()
    for copy in copies:
        copy.wait()


def on_device(
    tokens,
    mix_gain,
    w_query,
    w_forget,
    w_input,
    w_outgate,
    decay_floor,
    head_gain,
    prev_state,
    w_output,
    moe_gain,
    route_ids,
    route_logits,
    w_exp_gate,
    w_exp_up,
    w_exp_down,
):
    vmem = pl.BlockSpec(memory_space=pltpu.VMEM)
    hbm = pl.BlockSpec(memory_space=pltpu.HBM)
    dma = pltpu.SemaphoreType.DMA
    layer_out, new_state = pl.pallas_call(
        layer_kernel,
        name="layer",
        out_shape=(
            pltpu.VMEM((SEQ, WIDTH), BF),
            pltpu.VMEM((SEQ, HEADS, HEAD, HEAD), F32),
        ),
        in_specs=[hbm] * 17,
        out_specs=(vmem,) * 2,
        scratch_shapes=[
            pltpu.VMEM((SEQ, WIDTH), BF),
            pltpu.VMEM((1, WIDTH), F32),
            pltpu.VMEM((1, MIX), F32),
            pltpu.VMEM((1, HEAD), F32),
            pltpu.VMEM((1, WIDTH), F32),
            pltpu.VMEM((2, SEQ), jnp.int32),
            pltpu.VMEM((2, SEQ), F32),
            pltpu.VMEM((1, CHIPS * CAP), jnp.int32),
            pltpu.VMEM((WIDTH, MIX), BF),
            pltpu.VMEM((WIDTH, MIX), BF),
            pltpu.VMEM((WIDTH, MIX), BF),
            pltpu.VMEM((WIDTH, MIX), BF),
            pltpu.VMEM((SEQ, HEADS, HEAD, HEAD), F32),
            pltpu.VMEM((MIX, WIDTH), BF),
            pltpu.VMEM((WIDTH, HID), BF),
            pltpu.VMEM((WIDTH, HID), BF),
            pltpu.VMEM((HID, WIDTH), BF),
            pltpu.VMEM((SEQ, MIX), F32),
            pltpu.VMEM((SEQ, WIDTH), BF),
            pltpu.VMEM((SEQ, WIDTH), BF),
            pltpu.VMEM((SEQ, WIDTH), BF),
            pltpu.VMEM((SEQ, WIDTH), BF),
            pltpu.VMEM((EXPERTS, CAP, HALF), BF),
            pltpu.VMEM((2, CHIPS, CAP, HALF), BF),
            pltpu.VMEM((CHIPS * CAP, HALF), BF),
            pltpu.VMEM((CHIPS * CAP, HALF), BF),
            pltpu.VMEM((CHIPS, CAP, HALF), BF),
            pltpu.VMEM((CHIPS, CAP, HALF), BF),
            pltpu.VMEM((2, SEQ, HALF), BF),
            dma((8,)),
            dma((17,)),
            dma((4,)),
            dma((CHUNKS,)),
            dma((CHUNKS,)),
            dma((CHUNKS,)),
            dma((CHUNKS,)),
            dma((CHUNKS,)),
            dma((CHUNKS,)),
            dma((CHUNKS,)),
            dma((CHUNKS,)),
        ],
        compiler_params=pltpu.CompilerParams(
            collective_id=0, has_side_effects=True, vmem_limit_bytes=62750720
        ),
    )(
        tokens,
        mix_gain[None, :],
        decay_floor[None, :],
        head_gain[None, :],
        moe_gain[None, :],
        route_ids.T,
        route_logits.T,
        jnp.asarray(slot_table()),
        w_query,
        w_forget,
        w_input,
        w_outgate,
        prev_state,
        w_output,
        w_exp_gate,
        w_exp_up,
        w_exp_down,
    )
    return pl.pallas_call(
        deliver_kernel,
        name="deliver",
        out_shape=(
            jax.ShapeDtypeStruct((SEQ, WIDTH), BF),
            jax.ShapeDtypeStruct((SEQ, HEADS, HEAD, HEAD), F32),
        ),
        in_specs=[vmem, vmem],
        out_specs=(hbm, hbm),
        scratch_shapes=[dma((5,))],
        compiler_params=pltpu.CompilerParams(vmem_limit_bytes=6 * 1024 * 1024),
    )(layer_out, new_state)


def solution(mesh):
    placed = (
        P("ep", None),
        P(),
        P(None, "tp"),
        P(None, "tp"),
        P(None, "tp"),
        P(None, "tp"),
        P("tp"),
        P(),
        P("ep", "tp", None, None),
        P("tp", None),
        P(),
        P("ep", None),
        P("ep", None),
        P("ep", None, "tp"),
        P("ep", None, "tp"),
        P("ep", "tp", None),
    )
    return jax.shard_map(
        on_device,
        mesh=mesh,
        in_specs=placed,
        out_specs=(P("ep", None), P("ep", "tp", None, None)),
        check_vma=False,
    )
```

```python
import functools

import jax
import jax.numpy as jnp
import numpy as np
from jax import lax
from jax.experimental import pallas as pl
from jax.experimental.pallas import tpu as pltpu
from jax.sharding import PartitionSpec as P

MESH = pl.DeviceIdType.MESH
SIDE = 4
CHIPS = SIDE**3
EXPERTS = CHIPS // 2
CAP = 8
SIZES = (16, 16, 16, 16)
STARTS = tuple(sum(SIZES[:k]) for k in range(len(SIZES)))
CHUNKS = len(SIZES)
OWN = STARTS[-1]
SEQ = 16
WIDTH = 2048
HALF = WIDTH // 2
HEADS = 4
HEAD = 128
MIX = HEADS * HEAD
HID = 768
EPS = 1e-6
AHEAD = 6
MIX_LOADS = 14
BF = jnp.bfloat16
F32 = jnp.float32


def hops(offset):
    return sum(min(v, SIDE - v) for v in offset)


def offset_order():
    every = [(z, y, x) for z in range(SIDE) for y in range(SIDE) for x in range(SIDE)]
    order = sorted(every[1:], key=lambda o: ((sum(o) - 1) % SIDE, -hops(o), min(o, tuple(-v % SIDE for v in o)), o))
    order.insert(OWN, (0, 0, 0))
    return order


OFFSETS = offset_order()


def slot_table():
    packed = [z * 16 + y * 4 + x for z, y, x in OFFSETS]
    return np.repeat(np.array(packed, np.int32), CAP)[None, :]


def rms(values, gains):
    return values * lax.rsqrt(jnp.mean(values * values, axis=-1, keepdims=True) + EPS) * gains


def halves(src, dst):
    size = src.shape[0] // 2
    return [(src.at[pl.ds(i * size, size)], dst.at[pl.ds(i * size, size)]) for i in range(2)]


def layer_kernel(
    tokens_h,
    mix_gain_h,
    floor_h,
    head_gain_h,
    moe_gain_h,
    ids_h,
    logits_h,
    table_h,
    w_query,
    w_forget,
    w_input,
    w_outgate,
    prev,
    w_output,
    w_gate,
    w_up,
    w_down,
    out,
    new_state,
    tokens,
    mix_gain,
    floor,
    head_gain,
    moe_gain,
    ids_t,
    logits_t,
    table,
    wq_v,
    wf_v,
    wi_v,
    wg_v,
    prev_v,
    wo_v,
    eg_v,
    eu_v,
    ed_v,
    readout_v,
    part_own,
    part_sib,
    n2_v,
    middle_v,
    outgoing,
    inbox,
    down_send,
    down_recv,
    ret_out,
    ret_in,
    final,
    small_sem,
    load_sem,
    pair_sem,
    disp_send,
    disp_recv,
    fwd_send,
    fwd_recv,
    down_sems,
    down_recv_sems,
    ret_send,
    ret_recv,
):
    me = lax.axis_index("ep")
    c = lax.axis_index("tp")
    other = 1 - c
    z, y, x = lax.div(me, 16), lax.rem(lax.div(me, 4), 4), lax.rem(me, 4)
    z_to = [lax.rem(z + d, 4) * 16 for d in range(4)]
    y_to = [lax.rem(y + d, 4) * 4 for d in range(4)]
    x_to = [lax.rem(x + d, 4) for d in range(4)]

    def ahead(o):
        return z_to[o[0]] + y_to[o[1]] + x_to[o[2]]

    def behind(o):
        return z_to[-o[0] % 4] + y_to[-o[1] % 4] + x_to[-o[2] % 4]

    def to_sibling(src, dst, send, recv):
        return pltpu.make_async_remote_copy(
            src_ref=src, dst_ref=dst, send_sem=send, recv_sem=recv, device_id={"tp": other}, device_id_type=MESH
        )

    barrier = pltpu.get_barrier_semaphore()
    pl.semaphore_signal(barrier, inc=1, device_id={"tp": other}, device_id_type=MESH)
    for o in OFFSETS[:OWN] + OFFSETS[OWN + 1 :]:
        pl.semaphore_signal(barrier, inc=1, device_id={"ep": ahead(o)}, device_id_type=MESH)

    small = [
        pltpu.make_async_copy(src, dst, small_sem.at[i])
        for i, (src, dst) in enumerate(
            (
                (tokens_h, tokens),
                (mix_gain_h, mix_gain),
                (floor_h, floor),
                (head_gain_h, head_gain),
                (moe_gain_h, moe_gain),
                (ids_h, ids_t),
                (logits_h, logits_t),
                (table_h, table),
            )
        )
    ]
    parts = []
    for src, dst in ((w_forget, wf_v), (w_query, wq_v)):
        parts += halves(src, dst)
    parts += [(prev.at[pl.ds(4 * i, 4)], prev_v.at[pl.ds(4 * i, 4)]) for i in range(4)]
    for src, dst in ((w_input, wi_v), (w_outgate, wg_v), (w_output, wo_v)):
        parts += halves(src, dst)
    parts += [(w_gate.at[0], eg_v), (w_up.at[0], eu_v), (w_down.at[0], ed_v)]
    loads = [pltpu.make_async_copy(src, dst, load_sem.at[i]) for i, (src, dst) in enumerate(parts)]
    expert_loads = loads[MIX_LOADS:]

    def arrive(first, count):
        for i in range(first, first + count):
            loads[i].wait()
            if i + AHEAD < MIX_LOADS:
                loads[i + AHEAD].start()

    for copy in small:
        copy.start()
    for copy in loads[:AHEAD]:
        copy.start()
    for copy in small:
        copy.wait()

    residual = tokens[...].astype(F32)
    normed = rms(residual, mix_gain[...]).astype(BF)
    arrive(0, 2)
    forget_pre = jnp.dot(normed, wf_v[...], preferred_element_type=F32)
    low = floor[...]
    forget = low + (1.0 - low) * jax.nn.sigmoid(forget_pre)
    key = (1.0 - low) * jax.nn.sigmoid(-forget_pre)
    rows16 = lax.broadcasted_iota(jnp.int32, (SEQ, SEQ), 0)
    cols16 = lax.broadcasted_iota(jnp.int32, (SEQ, SEQ), 1)

    def column(row):
        return jnp.sum(jnp.where(rows16 == cols16, row, jnp.zeros_like(row)), axis=1, keepdims=True)

    ids_row = [ids_t[k : k + 1, :] for k in range(2)]
    ids_col = [column(row) for row in ids_row]

    def rank_col(k):
        same = (ids_col[k] == ids_row[0]).astype(jnp.int32) + (ids_col[k] == ids_row[1]).astype(jnp.int32)
        return jnp.sum(jnp.where(cols16 < rows16, same, 0), axis=1, keepdims=True)

    def rank_row(k):
        same = (ids_row[k] == ids_col[0]).astype(jnp.int32) + (ids_row[k] == ids_col[1]).astype(jnp.int32)
        return jnp.sum(jnp.where(rows16 < cols16, same, 0), axis=0, keepdims=True)

    slot_row = lax.broadcasted_iota(jnp.int32, (EXPERTS * CAP, SEQ), 0)
    disp = jnp.zeros((EXPERTS * CAP, SEQ), F32)
    for k in range(2):
        disp = jnp.where(slot_row == ids_row[k] * CAP + rank_row(k), 1.0, disp)
    disp = disp.astype(BF)

    tab = table[...]
    chip = (((tab >> 4) + z) & 3) * 16 + ((((tab >> 2) & 3) + y) & 3) * 4 + (((tab & 3) + x) & 3)
    slot_lane = lax.broadcasted_iota(jnp.int32, (1, CHIPS * CAP), 1)
    slot_key = (chip >> 1) * CAP + (slot_lane & (CAP - 1))
    comb = jnp.zeros((SEQ, CHIPS * CAP), F32)
    for k in range(2):
        weight = column(jax.nn.sigmoid(logits_t[k : k + 1, :] - logits_t[1 - k : 2 - k, :]))
        comb = jnp.where(slot_key == ids_col[k] * CAP + rank_col(k), weight, comb)
    comb_hi = comb.astype(BF)
    comb_lo = (comb - comb_hi.astype(F32)).astype(BF)
    comb = jnp.concatenate([comb_hi, comb_lo], axis=0)

    arrive(2, 2)
    query = jnp.dot(normed, wq_v[...], preferred_element_type=F32)
    query_forget = query * forget
    query_key = query * key
    columns = [query_forget[:, h * HEAD : (h + 1) * HEAD].T for h in range(HEADS)]
    for part in range(4):
        arrive(4 + part, 1)
        for s in range(4 * part, 4 * part + 4):
            for h in range(HEADS):
                lanes = slice(h * HEAD, (h + 1) * HEAD)
                readout_v[s : s + 1, lanes] = jnp.sum(columns[h][:, s : s + 1] * prev_v[s, h], axis=0, keepdims=True)
    arrive(8, 2)
    value = jnp.dot(normed, wi_v[...], preferred_element_type=F32)
    arrive(10, 2)
    outgate_pre = jnp.dot(normed, wg_v[...], preferred_element_type=F32)
    gate = outgate_pre * jax.nn.sigmoid(outgate_pre)
    gated = []
    for h in range(HEADS):
        lanes = slice(h * HEAD, (h + 1) * HEAD)
        dotted = jnp.sum(query_key[:, lanes], axis=1, keepdims=True)
        readout = readout_v[:, lanes] + dotted * value[:, lanes]
        gated.append((rms(readout, head_gain[...]) * gate[:, lanes]).astype(BF))
    gated = jnp.concatenate(gated, axis=1)
    arrive(12, 2)
    for copy in expert_loads:
        copy.start()
    part_own[...] = jnp.dot(gated, wo_v[...], preferred_element_type=F32).astype(BF)

    pl.semaphore_wait(barrier, CHIPS)
    swap = to_sibling(part_own, part_sib, pair_sem.at[0], pair_sem.at[1])
    swap.start()
    swap.wait()
    middle = (residual + (part_own[...].astype(F32) + part_sib[...].astype(F32))).astype(BF)
    middle_v[...] = middle
    n2_v[...] = rms(middle.astype(F32), moe_gain[...]).astype(BF)
    mine = pl.ds(pl.multiple_of(c * HALF, HALF), HALF)
    theirs = pl.ds(pl.multiple_of(other * HALF, HALF), HALF)
    rows = jnp.dot(disp, n2_v[:, mine], preferred_element_type=F32)
    outgoing[...] = rows.reshape(EXPERTS, CAP, HALF).astype(BF)

    def slots(ref, k, first=0):
        return ref.at[pl.ds(STARTS[k] + first, SIZES[k] - first)]

    def chunk_of(i):
        return max(k for k in range(CHUNKS) if STARTS[k] <= i)

    def wait_for(ref, k, sem):
        first = 1 if k == chunk_of(OWN) else 0
        pltpu.make_async_copy(slots(ref, k, first), slots(ref, k, first), sem).wait()

    for i, o in enumerate(OFFSETS):
        if i == OWN:
            continue
        to = ahead(o)
        pltpu.make_async_remote_copy(
            src_ref=outgoing.at[lax.div(to, 2)],
            dst_ref=inbox.at[c, i],
            send_sem=disp_send.at[chunk_of(i)],
            recv_sem=disp_recv.at[chunk_of(i)],
            device_id={"ep": to},
            device_id_type=MESH,
        ).start()
    inbox[c, OWN] = outgoing[lax.div(me, 2)]

    for h in range(HEADS):
        lanes = slice(h * HEAD, (h + 1) * HEAD)
        columns = forget[:, lanes].T
        for s in range(SEQ):
            vector = value[s : s + 1, lanes]
            new_state[s, h] = vector + columns[:, s : s + 1] * (prev_v[s, h] - vector)

    def rows_of(k):
        return pl.ds(STARTS[k] * CAP, SIZES[k] * CAP)

    def flat(values):
        return values.astype(F32).reshape(values.shape[0] * CAP, HALF).astype(BF)

    def finish(k):
        down_swaps[k].wait()
        total = own_down[k] + down_recv[rows_of(k)].astype(F32)
        ret_out[pl.ds(STARTS[k], SIZES[k])] = total.reshape(SIZES[k], CAP, HALF).astype(BF)
        for i in range(STARTS[k], STARTS[k] + SIZES[k]):
            if i == OWN:
                ret_in[OWN] = ret_out[OWN]
                continue
            pltpu.make_async_remote_copy(
                src_ref=ret_out.at[i],
                dst_ref=ret_in.at[i],
                send_sem=ret_send.at[k],
                recv_sem=ret_recv.at[k],
                device_id={"ep": behind(OFFSETS[i])},
                device_id_type=MESH,
            ).start()

    down_swaps, own_down = [], []
    for k in range(CHUNKS):
        wait_for(inbox.at[c], k, disp_recv.at[k])
        forward = to_sibling(slots(inbox.at[c], k), slots(inbox.at[c], k), fwd_send.at[k], fwd_recv.at[k])
        forward.start()
        if k == 0:
            for copy in expert_loads:
                copy.wait()
        rows = flat(inbox[c, pl.ds(STARTS[k], SIZES[k])])
        gate_pre = jnp.dot(rows, eg_v[mine, :], preferred_element_type=F32)
        up_pre = jnp.dot(rows, eu_v[mine, :], preferred_element_type=F32)
        if k > 0:
            finish(k - 1)
        forward.wait()
        rows = flat(inbox[other, pl.ds(STARTS[k], SIZES[k])])
        gate_pre = gate_pre + jnp.dot(rows, eg_v[theirs, :], preferred_element_type=F32)
        up_pre = up_pre + jnp.dot(rows, eu_v[theirs, :], preferred_element_type=F32)
        activated = (gate_pre * jax.nn.sigmoid(gate_pre) * up_pre).astype(BF)
        down_send[rows_of(k)] = jnp.dot(activated, ed_v[:, theirs], preferred_element_type=F32).astype(BF)
        swap = to_sibling(down_send.at[rows_of(k)], down_recv.at[rows_of(k)], down_sems.at[k], down_recv_sems.at[k])
        swap.start()
        down_swaps.append(swap)
        own_down.append(jnp.dot(activated, ed_v[:, mine], preferred_element_type=F32))
    finish(CHUNKS - 1)

    total = jnp.zeros((2 * SEQ, HALF), F32)
    for k in range(CHUNKS):
        wait_for(ret_in, k, ret_recv.at[k])
        total += jnp.dot(
            comb[:, STARTS[k] * CAP : (STARTS[k] + SIZES[k]) * CAP],
            flat(ret_in[pl.ds(STARTS[k], SIZES[k])]),
            preferred_element_type=F32,
        )
    expert_sum = total[:SEQ] + total[SEQ:]
    final[c] = (middle_v[:, mine].astype(F32) + expert_sum).astype(BF)
    swap = to_sibling(final.at[c], final.at[c], pair_sem.at[2], pair_sem.at[3])
    swap.start()
    swap.wait()
    out[:, :HALF] = final[0]
    out[:, HALF:] = final[1]
    for k in range(CHUNKS):
        wait_for(inbox.at[c], k, disp_send.at[k])
        wait_for(ret_in, k, ret_send.at[k])


def deliver_kernel(made, state, out, new_state, sem):
    copies = [pltpu.make_async_copy(made, out, sem.at[4])]
    for i in range(4):
        part = pl.ds(4 * i, 4)
        copies.append(pltpu.make_async_copy(state.at[part], new_state.at[part], sem.at[i]))
    for copy in copies:
        copy.start()
    for copy in copies:
        copy.wait()


def on_device(
    tokens,
    mix_gain,
    w_query,
    w_forget,
    w_input,
    w_outgate,
    decay_floor,
    head_gain,
    prev_state,
    w_output,
    moe_gain,
    route_ids,
    route_logits,
    w_exp_gate,
    w_exp_up,
    w_exp_down,
):
    vmem = pl.BlockSpec(memory_space=pltpu.VMEM)
    hbm = pl.BlockSpec(memory_space=pltpu.HBM)
    dma = pltpu.SemaphoreType.DMA
    layer_out, new_state = pl.pallas_call(
        layer_kernel,
        name="layer",
        out_shape=(
            pltpu.VMEM((SEQ, WIDTH), BF),
            pltpu.VMEM((SEQ, HEADS, HEAD, HEAD), F32),
        ),
        in_specs=[hbm] * 17,
        out_specs=(vmem,) * 2,
        scratch_shapes=[
            pltpu.VMEM((SEQ, WIDTH), BF),
            pltpu.VMEM((1, WIDTH), F32),
            pltpu.VMEM((1, MIX), F32),
            pltpu.VMEM((1, HEAD), F32),
            pltpu.VMEM((1, WIDTH), F32),
            pltpu.VMEM((2, SEQ), jnp.int32),
            pltpu.VMEM((2, SEQ), F32),
            pltpu.VMEM((1, CHIPS * CAP), jnp.int32),
            pltpu.VMEM((WIDTH, MIX), BF),
            pltpu.VMEM((WIDTH, MIX), BF),
            pltpu.VMEM((WIDTH, MIX), BF),
            pltpu.VMEM((WIDTH, MIX), BF),
            pltpu.VMEM((SEQ, HEADS, HEAD, HEAD), F32),
            pltpu.VMEM((MIX, WIDTH), BF),
            pltpu.VMEM((WIDTH, HID), BF),
            pltpu.VMEM((WIDTH, HID), BF),
            pltpu.VMEM((HID, WIDTH), BF),
            pltpu.VMEM((SEQ, MIX), F32),
            pltpu.VMEM((SEQ, WIDTH), BF),
            pltpu.VMEM((SEQ, WIDTH), BF),
            pltpu.VMEM((SEQ, WIDTH), BF),
            pltpu.VMEM((SEQ, WIDTH), BF),
            pltpu.VMEM((EXPERTS, CAP, HALF), BF),
            pltpu.VMEM((2, CHIPS, CAP, HALF), BF),
            pltpu.VMEM((CHIPS * CAP, HALF), BF),
            pltpu.VMEM((CHIPS * CAP, HALF), BF),
            pltpu.VMEM((CHIPS, CAP, HALF), BF),
            pltpu.VMEM((CHIPS, CAP, HALF), BF),
            pltpu.VMEM((2, SEQ, HALF), BF),
            dma((8,)),
            dma((17,)),
            dma((4,)),
            dma((CHUNKS,)),
            dma((CHUNKS,)),
            dma((CHUNKS,)),
            dma((CHUNKS,)),
            dma((CHUNKS,)),
            dma((CHUNKS,)),
            dma((CHUNKS,)),
            dma((CHUNKS,)),
        ],
        compiler_params=pltpu.CompilerParams(
            collective_id=0, has_side_effects=True, vmem_limit_bytes=62750720
        ),
    )(
        tokens,
        mix_gain[None, :],
        decay_floor[None, :],
        head_gain[None, :],
        moe_gain[None, :],
        route_ids.T,
        route_logits.T,
        jnp.asarray(slot_table()),
        w_query,
        w_forget,
        w_input,
        w_outgate,
        prev_state,
        w_output,
        w_exp_gate,
        w_exp_up,
        w_exp_down,
    )
    return pl.pallas_call(
        deliver_kernel,
        name="deliver",
        out_shape=(
            jax.ShapeDtypeStruct((SEQ, WIDTH), BF),
            jax.ShapeDtypeStruct((SEQ, HEADS, HEAD, HEAD), F32),
        ),
        in_specs=[vmem, vmem],
        out_specs=(hbm, hbm),
        scratch_shapes=[dma((5,))],
        compiler_params=pltpu.CompilerParams(vmem_limit_bytes=6 * 1024 * 1024),
    )(layer_out, new_state)


def solution(mesh):
    placed = (
        P("ep", None),
        P(),
        P(None, "tp"),
        P(None, "tp"),
        P(None, "tp"),
        P(None, "tp"),
        P("tp"),
        P(),
        P("ep", "tp", None, None),
        P("tp", None),
        P(),
        P("ep", None),
        P("ep", None),
        P("ep", None, "tp"),
        P("ep", None, "tp"),
        P("ep", "tp", None),
    )
    return jax.shard_map(
        on_device,
        mesh=mesh,
        in_specs=placed,
        out_specs=(P("ep", None), P("ep", "tp", None, None)),
        check_vma=False,
    )
```
